32 devices in a mesh: sp: 16 (over z, y, x), tp: 2 (over core).
Axes of the slice: x: 2, y: 2, z: 4, core: 2. Of those that a mesh axis runs over, the one named last changes fastest.
Arguments:
- tokens: bfloat16 [16384, 2048], P('sp', 'tp'), may hold values from -6 to 6
- norm_gain: float32 [2048], replicated, may hold values from 0.1 to 1.9
- w_query: bfloat16 [2048, 1024], P('sp', 'tp'), may hold values from -0.125 to 0.125
- w_key: bfloat16 [2048, 512], P('sp', 'tp'), may hold values from -0.125 to 0.125
- w_value: bfloat16 [2048, 512], P('sp', 'tp'), may hold values from -0.125 to 0.125
- w_glu_a: bfloat16 [2048, 1024], P('sp', 'tp'), may hold values from -0.125 to 0.125
- w_glu_b: bfloat16 [2048, 1024], P('sp', 'tp'), may hold values from -0.125 to 0.125
- q_gain: float32 [64], replicated, may hold values from 0.8 to 7
- k_gain: float32 [64], replicated, may hold values from 0.8 to 7
- sink_logit: float32 [16], P('tp'), may hold values from 1 to 4
- conv_taps: float32 [31, 1024], P(None, 'tp'), may hold values from -1 to 1
- chan_gain: float32 [1024], P('tp'), may hold values from 0.1 to 1.9
- chan_bias: float32 [1024], P('tp'), may hold values from -3 to 3
- w_attn_back: bfloat16 [2048, 1024], P('sp', 'tp'), may hold values from -0.1875 to 0.1875
- w_conv_back: bfloat16 [2048, 1024], P('sp', 'tp'), may hold values from -0.1875 to 0.1875
Outputs:
- mixed: bfloat16 [16384, 2048], P(('sp', 'tp'))
- log_weight: float32 [16, 16384], P('tp', 'sp')
The draws below stay inside these ranges and needn't reach their ends.
All inputs are finite; a program needn't handle non-finite values.
Results may differ from the reference program's by a relative error of at most 0.014.
The reference program's roundings to bfloat16 on the way count: a program that leaves them out, or rounds other values in their place, can miss the bound.
Values may be sent and summed in bfloat16 or wider, within the bound.
A program may use at most 128 MiB of HBM per device.

```python
import jax
import jax.numpy as jnp
from jax import lax

D = 2048
HEAD = 64
Q_HEADS = 16
KV_HEADS = 8
CH = 1024
KW = 31
WINDOW = 128
TOKENS = 16384
N_TP = 2


def draw_q_gain(key, part):
    own_key = jax.random.fold_in(key, 11)
    return jax.random.uniform(own_key, (HEAD,), jnp.float32, 0.8, 1.2)


def draw_k_gain(key, part):
    own_key = jax.random.fold_in(key, 23)
    return jax.random.uniform(own_key, (HEAD,), jnp.float32, 0.8, 1.2)


def levels(rng, dims, split, least, high):
    gain = 1.0
    for dim, parts in split:
        draws = jax.random.uniform(jax.random.fold_in(jax.random.fold_in(rng, 6), dim), (parts,), jnp.float32, least / len(split), high / len(split))
        gain = gain * jnp.repeat(jnp.exp(draws), dims[dim] // parts).reshape((-1,) + (1,) * (len(dims) - 1 - dim))
    return gain


def normal_values(rng, extent, deviation, most, shards=(), held_as=jnp.bfloat16):
    drawn = deviation * jax.random.normal(rng, extent, jnp.float32)
    if shards:
        drawn = drawn * levels(rng, extent, shards, -0.22, 0.18)
    return jnp.clip(drawn, -most, most).astype(held_as)


def setup_inputs(seed: int = 0) -> dict:
    streams_of = jax.random.split(jax.random.key(seed), 16)
    return {
        "tokens": normal_values(streams_of[0], (TOKENS, D), 1.0, 6.0, ((0, 16), (1, 2))),
        "norm_gain": jnp.clip(1.0 + 0.18 * jax.random.normal(streams_of[1], (D,), jnp.float32), 0.1, 1.9),
        "w_query": normal_values(streams_of[2], (D, Q_HEADS * HEAD), D ** -0.5, 0.125, ((0, 16), (1, 2))),
        "w_key": normal_values(streams_of[3], (D, KV_HEADS * HEAD), D ** -0.5, 0.125, ((0, 16), (1, 2))),
        "w_value": normal_values(streams_of[4], (D, KV_HEADS * HEAD), D ** -0.5, 0.125, ((0, 16), (1, 2))),
        "w_glu_a": normal_values(streams_of[5], (D, CH), D ** -0.5, 0.125, ((0, 16), (1, 2))),
        "w_glu_b": normal_values(streams_of[6], (D, CH), D ** -0.5, 0.125, ((0, 16), (1, 2))),
        "q_gain": draw_q_gain(jax.random.fold_in(streams_of[15], 71), 0),
        "k_gain": draw_k_gain(jax.random.fold_in(streams_of[15], 71), 0),
        "sink_logit": jnp.clip(1.0 + 3.0 * jax.random.uniform(streams_of[9], (Q_HEADS,), jnp.float32) ** levels(streams_of[9], (Q_HEADS,), ((0, 2),), -0.2, 0.2), 1.0, 4.0),
        "conv_taps": normal_values(streams_of[10], (KW, CH), KW ** -0.5, 1.0, ((1, 2),), jnp.float32),
        "chan_gain": jnp.clip(1.0 + 0.18 * jax.random.normal(streams_of[11], (CH,), jnp.float32), 0.1, 1.9),
        "chan_bias": normal_values(streams_of[12], (CH,), 0.5, 3.0, ((0, 2),), jnp.float32),
        "w_attn_back": normal_values(streams_of[13], (D, Q_HEADS * HEAD), (Q_HEADS * HEAD) ** -0.5, 0.1875, ((0, 16), (1, 2))),
        "w_conv_back": normal_values(streams_of[14], (D, CH), CH ** -0.5, 0.1875, ((0, 16), (1, 2))),
    }


EPS = 1e-06

def row_norm(inputs, scale_vec):
    squares = lax.optimization_barrier(jnp.mean(inputs * inputs, axis=-1, keepdims=True))
    return inputs * lax.rsqrt(squares + EPS) * scale_vec

def reference(tokens, norm_gain, w_query, w_key, w_value, w_glu_a, w_glu_b, q_gain, k_gain, sink_logit, conv_taps, chan_gain, chan_bias, w_attn_back, w_conv_back):
    seq_total = tokens.shape[0]
    group_size = Q_HEADS // KV_HEADS
    normed = row_norm(tokens.astype(jnp.float32), norm_gain).astype(jnp.bfloat16)
    query_raw = jnp.dot(normed, w_query, preferred_element_type=jnp.float32)
    key_raw = jnp.dot(normed, w_key, preferred_element_type=jnp.float32)
    value_raw = jnp.dot(normed, w_value, preferred_element_type=jnp.float32)
    glu_a = jnp.dot(normed, w_glu_a, preferred_element_type=jnp.float32)
    glu_b = jnp.dot(normed, w_glu_b, preferred_element_type=jnp.float32)
    queries = row_norm(query_raw.reshape(seq_total, Q_HEADS, HEAD), q_gain).astype(jnp.bfloat16)
    key_rows = row_norm(key_raw.reshape(seq_total, KV_HEADS, HEAD), k_gain).astype(jnp.bfloat16)
    value_rows = value_raw.astype(jnp.bfloat16).reshape(seq_total, KV_HEADS, HEAD)
    gated_rows = (glu_a * jax.nn.sigmoid(glu_b)).astype(jnp.bfloat16)
    zero_keys = jnp.zeros((WINDOW, KV_HEADS, HEAD), jnp.bfloat16)
    keys_padded = jnp.concatenate([zero_keys, key_rows], 0)
    values_padded = jnp.concatenate([zero_keys, value_rows], 0)
    offsets = jnp.arange(WINDOW, dtype=jnp.int32)
    band_offsets = jnp.arange(2 * WINDOW, dtype=jnp.int32)
    distance = WINDOW + offsets[:, None] - band_offsets[None, :]
    allowed = (distance >= 0) & (distance < WINDOW)
    sink_table = sink_logit.reshape(KV_HEADS, group_size)[:, :, None, None]

    def one_block(block_index):
        block_start = (block_index * WINDOW).astype(jnp.int32)
        query_block = lax.dynamic_slice_in_dim(queries, block_start, WINDOW, 0).astype(jnp.float32)
        query_block = query_block.reshape(WINDOW, KV_HEADS, group_size, HEAD)
        key_band = lax.dynamic_slice_in_dim(keys_padded, block_start, 2 * WINDOW, 0).astype(jnp.float32)
        value_band = lax.dynamic_slice_in_dim(values_padded, block_start, 2 * WINDOW, 0).astype(jnp.float32)
        scores = jnp.einsum('qhgd,khd->hgqk', query_block, key_band) * HEAD ** (-0.5)
        visible = allowed & (block_start - WINDOW + band_offsets[None, :] >= 0)
        masked = jnp.where(visible, scores, -jnp.inf)
        largest = jnp.maximum(lax.optimization_barrier(jnp.max(masked, axis=-1, keepdims=True)), sink_table)
        weights = jnp.where(visible, jnp.exp(scores - largest), 0.0)
        weight_sum = lax.optimization_barrier(jnp.sum(weights, axis=-1, keepdims=True)) + jnp.exp(sink_table - largest)
        log_sum = (largest + jnp.log(weight_sum))[..., 0].reshape(Q_HEADS, WINDOW)
        probabilities = (weights / weight_sum).astype(jnp.bfloat16)
        mixed_rows = jnp.einsum('hgqk,khd->qhgd', probabilities.astype(jnp.float32), value_band)
        return (mixed_rows.astype(jnp.bfloat16).reshape(WINDOW, Q_HEADS * HEAD), log_sum)
    block_count = seq_total // WINDOW
    attended, log_sums = lax.map(one_block, jnp.arange(block_count, dtype=jnp.int32))
    attended = attended.reshape(seq_total, Q_HEADS * HEAD)
    log_weight = jnp.transpose(log_sums, (1, 0, 2)).reshape(Q_HEADS, seq_total)
    zero_rim = jnp.zeros((KW - 1, CH), jnp.float32)
    extended = jnp.concatenate([zero_rim, gated_rows.astype(jnp.float32)], 0)
    convolved = jnp.zeros((seq_total, CH), jnp.float32)
    for tap_index in range(KW):
        convolved = convolved + conv_taps[tap_index] * extended[tap_index:tap_index + seq_total]
    center = lax.optimization_barrier(jnp.mean(convolved, axis=-1, keepdims=True))
    spread = lax.optimization_barrier(jnp.mean(convolved * convolved, axis=-1, keepdims=True)) - center * center
    normal = (convolved - center) * lax.rsqrt(spread + EPS) * chan_gain + chan_bias
    conv_rows = jax.nn.silu(normal).astype(jnp.bfloat16)
    attn_cols = Q_HEADS * HEAD // N_TP
    conv_cols = CH // N_TP
    summed = jnp.zeros((seq_total, D), jnp.float32)
    for shard_index in range(N_TP):
        attn_lo = shard_index * attn_cols
        conv_lo = shard_index * conv_cols
        partial_sum = jnp.dot(attended[:, attn_lo:attn_lo + attn_cols], w_attn_back[:, attn_lo:attn_lo + attn_cols].T, preferred_element_type=jnp.float32)
        partial_sum = partial_sum + jnp.dot(conv_rows[:, conv_lo:conv_lo + conv_cols], w_conv_back[:, conv_lo:conv_lo + conv_cols].T, preferred_element_type=jnp.float32)
        rounded = lax.optimization_barrier(partial_sum.astype(jnp.bfloat16))
        summed = summed + rounded.astype(jnp.float32)
    return (summed.astype(jnp.bfloat16), log_weight)
```

```python
import functools
import itertools

import jax
import jax.numpy as jnp
from jax import lax
from jax.experimental import pallas as pl
from jax.experimental.pallas import tpu as pltpu
from jax.sharding import PartitionSpec as P

HEAD = 64
CH = 1024
KW = 31
WINDOW = 128


EPS = 1e-06


def passed_along(value, axis, steps):
    count = lax.axis_size(axis)
    leading, last = (max(0, -steps), min(count, count - steps))
    return lax.ppermute(value, axis, [(source, source + steps) for source in range(leading, last)])


def row_norm(inputs, scale_vec):
    squares = jnp.mean(inputs * inputs, axis=-1, keepdims=True)
    return inputs * lax.rsqrt(squares + EPS) * scale_vec


MESH = pl.DeviceIdType.MESH
ORDERS = ("xzy", "yzx", "xzy", "yzx", "zxy", "zyx")
STARTS = (0, 0, 1, 1, 2, 2)
BLOCK = 256


def gather_kernel(
    n_sp, n_tp, tok, gain, wa, wb, wq, wkv, wo, wc, gated, query, key_value, back,
    rows_full, fa, fb, fq, fkv, recv, send, tok_recv, tok_send, own_sem,
):
    me, core = lax.axis_index("sp"), lax.axis_index("tp")
    depth = n_sp // 4
    x, y, z = me % 2, (me // 2) % 2, me // 4
    near = {
        "x": (me - x + (1 - x), None),
        "y": (me - 2 * y + 2 * (1 - y), None),
        "up": (me + 4, z < depth - 1),
        "down": (me - 4, z > 0),
    }
    lanes = {name: index for index, name in enumerate(near)}
    shards = (wa, wb, wq, wkv, wo, wc)
    shard_rows, width = wa.shape
    wholes = (fa, fb, fq, fkv, back.at[:, pl.ds(0, width)], back.at[:, pl.ds(width, width)])

    def guarded(conditions, action):
        known = [condition for condition in conditions if condition is not None]
        if not known:
            action()
        else:
            pl.when(functools.reduce(jnp.logical_and, known))(action)

    barrier = pltpu.get_barrier_semaphore()
    for name, (target, exists) in near.items():
        guarded((exists,), lambda target=target: pl.semaphore_signal(
            barrier, inc=1, device_id=(target, core), device_id_type=MESH))
    for step in range(1, n_tp):
        pl.semaphore_signal(
            barrier, inc=1, device_id=(me, lax.rem(core + step, n_tp)), device_id_type=MESH)
    ends = jnp.where(z < depth - 1, 1, 0) + jnp.where(z > 0, 1, 0)
    pl.semaphore_wait(barrier, 2 + (n_tp - 1) + ends)

    tok_width = tok.shape[1]

    def tok_columns(owner):
        return rows_full.at[:, pl.ds(pl.multiple_of(owner * tok_width, tok_width), tok_width)]

    def tok_copy(step):
        return pltpu.make_async_remote_copy(
            src_ref=tok, dst_ref=tok_columns(core),
            send_sem=tok_send.at[step - 1], recv_sem=tok_recv.at[step - 1],
            device_id=(me, lax.rem(core + step, n_tp)), device_id_type=MESH)

    def spot(chunk, owner):
        return wholes[chunk].at[pl.ds(pl.multiple_of(owner * shard_rows, shard_rows), shard_rows), :]

    def block_copy(chunk, owner, name, own):
        return pltpu.make_async_remote_copy(
            src_ref=shards[chunk] if own else spot(chunk, owner),
            dst_ref=spot(chunk, owner),
            send_sem=send.at[chunk, owner, lanes[name]], recv_sem=recv.at[chunk, owner],
            device_id=(near[name][0], core), device_id_type=MESH)

    def blocks(chunk):
        order = ORDERS[chunk]
        for dx, dy, dz in itertools.product((0, 1), (0, 1), range(1 - depth, depth)):
            moved = {"x": dx, "y": dy, "z": dz}
            last = max([order.index(axis) for axis in order if moved[axis]], default=-1)
            onward = []
            for place, axis in enumerate(order):
                if axis == "z":
                    if place > last or (place == last and dz < 0):
                        onward.append("up")
                    if place > last or (place == last and dz > 0):
                        onward.append("down")
                elif place > last:
                    onward.append(axis)
            owner = (z + dz) * 4 + jnp.where(y == 0, dy, 1 - dy) * 2 + jnp.where(x == 0, dx, 1 - dx)
            inside = None if dz == 0 else (z + dz >= 0 if dz < 0 else z + dz < depth)
            yield dx + dy + abs(dz), owner, inside, onward

    plan = [sorted(blocks(chunk), key=lambda item: item[0]) for chunk in range(len(shards))]
    hops = depth + 1

    def relay(chunk, hop):
        for distance, owner, inside, onward in plan[chunk]:
            if distance != hop:
                continue

            def step(owner=owner, onward=onward):
                if hop:
                    block_copy(chunk, owner, "x", False).wait_recv()
                for name in onward:
                    guarded((near[name][1],), lambda name=name: block_copy(
                        chunk, owner, name, hop == 0).start())
            guarded((inside,), step)

    own_copies = [
        pltpu.make_async_copy(shards[chunk], spot(chunk, me), own_sem.at[chunk])
        for chunk in range(len(shards))
    ] + [pltpu.make_async_copy(tok, tok_columns(core), own_sem.at[len(shards)])]

    row_blocks = tok.shape[0] // BLOCK

    def row_slice(index):
        return pl.ds(pl.multiple_of(index * BLOCK, BLOCK), BLOCK)

    def normalise():
        for step in range(1, n_tp):
            tok_copy(step).wait_recv()

        @pl.loop(0, tok.shape[0] // 64)
        def _(index):
            rows = pl.ds(pl.multiple_of(index * 64, 64), 64)
            rows_full[rows, :] = row_norm(
                rows_full[rows, :].astype(jnp.float32), gain[...]).astype(jnp.bfloat16)

    def project(weights):
        def dot(rows, weight):
            return jnp.dot(rows_full[rows, :], weight[...], preferred_element_type=jnp.float32)

        @pl.loop(0, row_blocks)
        def _(index):
            rows = row_slice(index)
            if weights == "gate":
                gated[rows, :] = (dot(rows, fa) * jax.nn.sigmoid(dot(rows, fb))).astype(jnp.bfloat16)
            elif weights == "query":
                query[rows, :] = dot(rows, fq)
            else:
                key_value[rows, :] = dot(rows, fkv)

    after = {1: "gate", 2: "query", 3: "key_value"}
    for tick in range(max(STARTS) + hops + 1):
        for chunk, start in enumerate(STARTS):
            if 0 <= tick - start <= hops:
                relay(chunk, tick - start)
        if tick == 0:
            for step in range(1, n_tp):
                tok_copy(step).start()
            for copy in own_copies:
                copy.start()
            for copy in own_copies:
                copy.wait()
            normalise()
        for chunk, start in enumerate(STARTS):
            if tick - start == hops and chunk in after:
                project(after[chunk])
    for step in range(1, n_tp):
        tok_copy(step).wait_send()
    for chunk in range(len(shards)):
        for distance, owner, inside, onward in plan[chunk]:
            for name in onward:
                guarded((inside, near[name][1]), lambda chunk=chunk, owner=owner, name=name,
                        own=distance == 0: block_copy(chunk, owner, name, own).wait_send())


def gather_and_project(tokens, norm_gain, wa, wb, wq, wkv, wo, wc):
    n_sp, n_tp = lax.axis_size("sp"), lax.axis_size("tp")
    rows, features = tokens.shape[0], tokens.shape[1] * n_tp
    model, width = wa.shape[0] * n_sp, wa.shape[1]
    vmem = pl.BlockSpec(memory_space=pltpu.VMEM)
    return pl.pallas_call(
        functools.partial(gather_kernel, n_sp, n_tp),
        out_shape=(
            jax.ShapeDtypeStruct((rows, width), jnp.bfloat16),
            jax.ShapeDtypeStruct((rows, width), jnp.float32),
            jax.ShapeDtypeStruct((rows, wkv.shape[1]), jnp.float32),
            jax.ShapeDtypeStruct((model, 2 * width), jnp.bfloat16),
        ),
        in_specs=[vmem] * 8,
        out_specs=(vmem, vmem, vmem, pl.BlockSpec(memory_space=pl.ANY)),
        scratch_shapes=[pltpu.VMEM((rows, features), jnp.bfloat16)]
        + [pltpu.VMEM((model, width), jnp.bfloat16)] * 4
        + [
            pltpu.SemaphoreType.DMA((6, n_sp)),
            pltpu.SemaphoreType.DMA((6, n_sp, 4)),
            pltpu.SemaphoreType.DMA((n_tp - 1,)),
            pltpu.SemaphoreType.DMA((n_tp - 1,)),
            pltpu.SemaphoreType.DMA((7,)),
        ],
        compiler_params=pltpu.CompilerParams(collective_id=0, has_side_effects=True),
    )(tokens, norm_gain.reshape(1, features), wa, wb, wq, wkv, wo, wc)


def local(
    tokens,
    norm_gain,
    w_query,
    w_key,
    w_value,
    w_glu_a,
    w_glu_b,
    q_gain,
    k_gain,
    sink_logit,
    conv_taps,
    chan_gain,
    chan_bias,
    w_attn_back,
    w_conv_back,
):
    row_count = tokens.shape[0]
    q_local = w_query.shape[1] // HEAD
    kv_local = w_key.shape[1] // HEAD
    group_size = q_local // kv_local
    kv_width = kv_local * HEAD
    gated_rows, query_raw, key_value_raw, back = gather_and_project(
        tokens, norm_gain, w_glu_a, w_glu_b, w_query,
        jnp.concatenate([w_key, w_value], 1), w_attn_back, w_conv_back,
    )
    key_raw, value_raw = key_value_raw[:, :kv_width], key_value_raw[:, kv_width:]
    queries = row_norm(query_raw.reshape(row_count, q_local, HEAD), q_gain).astype(jnp.bfloat16)
    key_rows = (
        row_norm(key_raw.reshape(row_count, kv_local, HEAD), k_gain)
        .astype(jnp.bfloat16)
        .reshape(row_count, kv_width)
    )
    value_rows = value_raw.astype(jnp.bfloat16)
    key_value = jnp.concatenate([key_rows, value_rows], 1)
    key_value_rim = passed_along(key_value[row_count - WINDOW :], "sp", 1)
    gated_rim = passed_along(gated_rows[row_count - (KW - 1) :], "sp", 1)
    block_count = row_count // WINDOW
    extended = jnp.concatenate([key_value_rim, key_value], 0).reshape(
        block_count + 1, WINDOW, 2 * kv_width
    )
    band = jnp.concatenate([extended[:-1], extended[1:]], 1)
    key_band = band[:, :, :kv_width].reshape(block_count, 2 * WINDOW, kv_local, HEAD)
    value_band = band[:, :, kv_width:].reshape(block_count, 2 * WINDOW, kv_local, HEAD)
    grouped = queries.reshape(block_count, WINDOW, kv_local, group_size, HEAD)
    scores = jnp.einsum(
        "nqhgd,nkhd->nhgqk", grouped, key_band, preferred_element_type=jnp.float32
    ) * HEAD ** (-0.5)
    offsets = jnp.arange(WINDOW, dtype=jnp.int32)
    band_offsets = jnp.arange(2 * WINDOW, dtype=jnp.int32)
    distance = WINDOW + offsets[:, None] - band_offsets[None, :]
    allowed = (distance >= 0) & (distance < WINDOW)
    anchor = lax.axis_index("sp") * row_count
    key_position = (
        anchor
        + jnp.arange(block_count, dtype=jnp.int32)[:, None] * WINDOW
        - WINDOW
        + band_offsets[None, :]
    )
    visible = (allowed[None, :, :] & (key_position[:, None, :] >= 0))[:, None, None]
    sink_table = sink_logit.reshape(kv_local, group_size)[None, :, :, None, None]
    masked = jnp.where(visible, scores, -jnp.inf)
    largest = jnp.maximum(jnp.max(masked, axis=-1, keepdims=True), sink_table)
    weights = jnp.where(visible, jnp.exp(scores - largest), 0.0)
    weight_sum = jnp.sum(weights, axis=-1, keepdims=True) + jnp.exp(sink_table - largest)
    log_weight = (largest + jnp.log(weight_sum))[..., 0]
    log_weight = jnp.transpose(log_weight, (1, 2, 0, 3)).reshape(q_local, row_count)
    probabilities = (weights / weight_sum).astype(jnp.bfloat16)
    attended = jnp.einsum(
        "nhgqk,nkhd->nqhgd", probabilities, value_band, preferred_element_type=jnp.float32
    )
    attended = attended.astype(jnp.bfloat16).reshape(row_count, q_local * HEAD)
    gate_extended = jnp.concatenate([gated_rim, gated_rows], 0).astype(jnp.float32)
    convolved = jnp.zeros((row_count, gated_rows.shape[1]), jnp.float32)
    for tap_index in range(KW):
        convolved = (
            convolved + conv_taps[tap_index] * gate_extended[tap_index : tap_index + row_count]
        )
    channel_sums = lax.psum(
        (jnp.sum(convolved, axis=1), jnp.sum(convolved * convolved, axis=1)), "tp"
    )
    center = (channel_sums[0] / CH)[:, None]
    spread = (channel_sums[1] / CH)[:, None] - center * center
    conv_rows = jax.nn.silu(
        (convolved - center) * lax.rsqrt(spread + EPS) * chan_gain + chan_bias
    ).astype(jnp.bfloat16)
    both = jnp.concatenate([attended, conv_rows], 1)
    contract = (((1,), (1,)), ((), ()))

    def mixed(rows):
        return lax.dot_general(rows, back, contract, preferred_element_type=jnp.float32).astype(
            jnp.bfloat16
        )

    n_tp = lax.axis_size("tp")
    if n_tp == 2:
        half = row_count // 2
        core = lax.axis_index("tp")
        theirs = mixed(lax.dynamic_slice_in_dim(both, (1 - core) * half, half, 0))
        arrived = lax.ppermute(theirs, "tp", [(0, 1), (1, 0)])
        ours = mixed(lax.dynamic_slice_in_dim(both, core * half, half, 0))
        summed = (ours.astype(jnp.float32) + arrived.astype(jnp.float32)).astype(jnp.bfloat16)
    else:
        summed = lax.psum_scatter(mixed(both), "tp", scatter_dimension=0, tiled=True)
    return (summed, log_weight)


def solution(mesh):
    placed = (
        P("sp", "tp"),
        P(),
        P("sp", "tp"),
        P("sp", "tp"),
        P("sp", "tp"),
        P("sp", "tp"),
        P("sp", "tp"),
        P(),
        P(),
        P("tp"),
        P(None, "tp"),
        P("tp"),
        P("tp"),
        P("sp", "tp"),
        P("sp", "tp"),
    )
    return jax.shard_map(
        local,
        mesh=mesh,
        in_specs=placed,
        out_specs=(P(("sp", "tp"), None), P("tp", "sp")),
        check_vma=False,
    )
```
